32 devices in a mesh: kv: 8 (over z, y), tp: 4 (over x, core).
Axes of the slice: x: 2, y: 2, z: 4, core: 2. Of those that a mesh axis runs over, the one named last changes fastest.
Arguments:
- block_in: bfloat16 [64, 4096], P(None, ('kv', 'tp')), may hold values from -30 to 30
- before_gain: bfloat16 [4096], P('kv'), may hold values from 0.099609375 to 1.8984375
- before_gate: bfloat16 [4096, 11264], P('kv', 'tp'), may hold values from -0.09375 to 0.09375
- before_up: bfloat16 [4096, 11264], P('kv', 'tp'), may hold values from -0.09375 to 0.09375
- before_down: bfloat16 [11264, 4096], P('tp', 'kv'), may hold values from -0.0546875 to 0.0546875
- mix_gain: bfloat16 [4096], P('kv'), may hold values from 0.099609375 to 1.8984375
- input_gate: bfloat16 [4096, 8192], P('kv', 'tp'), may hold values from -0.09375 to 0.09375
- input_value: bfloat16 [4096, 8192], P('kv', 'tp'), may hold values from -0.09375 to 0.09375
- input_write: bfloat16 [4096, 2048], P('kv', 'tp'), may hold values from -0.09375 to 0.09375
- input_read: bfloat16 [4096, 2048], P('kv', 'tp'), may hold values from -0.09375 to 0.09375
- input_step: bfloat16 [4096, 128], P('kv', 'tp'), may hold values from -0.09375 to 0.09375
- step_bias: float32 [128], P('tp'), may hold values from -3 to 0
- decay_log: float32 [128], P('tp'), may hold values from -1 to 1.4
- skip_gain: float32 [128], P('tp'), may hold values from 0.5 to 2
- value_taps: bfloat16 [4, 8192], P(None, 'tp'), may hold values from -3 to 3
- write_taps: bfloat16 [4, 2048], P(None, 'tp'), may hold values from -3 to 3
- read_taps: bfloat16 [4, 2048], P(None, 'tp'), may hold values from -3 to 3
- value_window: bfloat16 [64, 3, 8192], P('kv', None, 'tp'), may hold values from -6 to 6
- write_window: bfloat16 [64, 3, 2048], P('kv', None, 'tp'), may hold values from -6 to 6
- read_window: bfloat16 [64, 3, 2048], P('kv', None, 'tp'), may hold values from -6 to 6
- scan_state: float32 [64, 128, 64, 128], P('kv', 'tp'), may hold values from -2 to 2
- group_gain: bfloat16 [8192], P('tp'), may hold values from 0.099609375 to 1.8984375
- mixer_out: bfloat16 [8192, 4096], P('tp', 'kv'), may hold values from -0.0625 to 0.0625
- after_gain: bfloat16 [4096], P('kv'), may hold values from 0.099609375 to 1.8984375
- after_gate: bfloat16 [4096, 11264], P('kv', 'tp'), may hold values from -0.09375 to 0.09375
- after_up: bfloat16 [4096, 11264], P('kv', 'tp'), may hold values from -0.09375 to 0.09375
- after_down: bfloat16 [11264, 4096], P('tp', 'kv'), may hold values from -0.0546875 to 0.0546875
Outputs:
- block_out: bfloat16 [64, 4096], P(None, ('kv', 'tp'))
- state_next: float32 [64, 128, 64, 128], P('kv', 'tp')
- value_next: bfloat16 [64, 3, 8192], P('kv', None, 'tp')
- write_next: bfloat16 [64, 3, 2048], P('kv', None, 'tp')
- read_next: bfloat16 [64, 3, 2048], P('kv', None, 'tp')
The draws below stay inside these ranges and needn't reach their ends.
All inputs are finite; a program needn't handle non-finite values.
Results may differ from the reference program's by a relative error of at most 0.0085.
Values may be sent and summed in bfloat16 or wider, within the bound.
A program may use at most 128 MiB of HBM per device.

```python
import math
import jax
import jax.numpy as jnp
from jax import lax

D = 4096
FF = 11264
INNER = 8192
HEAD_DIM = 64
HEADS = 128
GROUPS = 16
STATE = 128
CONV = 4
BATCH = 64
N_KV = 8
N_TP = 4


def draw_block_in(key, part):
    base_key = jax.random.fold_in(key, 11)
    first_key, second_key = jax.random.split(base_key, 2)
    columns = jnp.arange(D, dtype=jnp.int32)
    column_block = D // (N_KV * N_TP)
    tp_place = (columns // column_block % N_TP).astype(jnp.float32)
    column_scale = jnp.exp(1.6 * columns.astype(jnp.float32) / D + 0.7 * tp_place / max(N_TP - 1, 1))
    row_scale = jnp.exp(jax.random.uniform(second_key, (BATCH, 1), jnp.float32, 0.0, 1.1))
    values = jnp.clip(jax.random.normal(first_key, (BATCH, D), jnp.float32), -4.0, 4.0)
    return (0.25 * values * row_scale * column_scale[None, :]).astype(jnp.bfloat16)


def shard_levels(own_key, extent, shards, low, largest):
    loudness = 1.0
    for position, parts in shards:
        heights = jax.random.uniform(jax.random.fold_in(jax.random.fold_in(own_key, 6), position), (parts,), jnp.float32, low / len(shards), largest / len(shards))
        loudness = loudness * jnp.repeat(jnp.exp(heights), extent[position] // parts).reshape((-1,) + (1,) * (len(extent) - 1 - position))
    return loudness


def centred(stream_key, extent, spread, reach, shards=(), kind=jnp.bfloat16):
    entries = spread * jax.random.normal(stream_key, extent, jnp.float32)
    if shards:
        entries = entries * shard_levels(stream_key, extent, shards, -0.22, 0.18)
    return jnp.clip(entries, -reach, reach).astype(kind)


def setup_inputs(seed: int = 0) -> dict:
    arg_keys = jax.random.split(jax.random.key(seed), 28)
    block_in = draw_block_in(jax.random.fold_in(arg_keys[27], 71), 0)
    before_gain = jnp.clip(1.0 + 0.18 * jax.random.normal(arg_keys[1], (D,), jnp.float32), 0.099609375, 1.8984375).astype(jnp.bfloat16)
    before_gate = centred(arg_keys[2], (D, FF), D ** -0.5, 0.09375, ((0, 8), (1, 4)))
    before_up = centred(arg_keys[3], (D, FF), D ** -0.5, 0.09375, ((0, 8), (1, 4)))
    before_down = centred(arg_keys[4], (FF, D), FF ** -0.5, 0.0546875, ((0, 4), (1, 8)))
    mix_gain = jnp.clip(1.0 + 0.18 * jax.random.normal(arg_keys[5], (D,), jnp.float32), 0.099609375, 1.8984375).astype(jnp.bfloat16)
    input_gate = centred(arg_keys[6], (D, INNER), D ** -0.5, 0.09375, ((0, 8), (1, 4)))
    input_value = centred(arg_keys[7], (D, INNER), D ** -0.5, 0.09375, ((0, 8), (1, 4)))
    input_write = centred(arg_keys[8], (D, GROUPS * STATE), D ** -0.5, 0.09375, ((0, 8), (1, 4)))
    input_read = centred(arg_keys[9], (D, GROUPS * STATE), D ** -0.5, 0.09375, ((0, 8), (1, 4)))
    input_step = centred(arg_keys[10], (D, HEADS), D ** -0.5, 0.09375, ((0, 8), (1, 4)))
    step_bias = jnp.clip(-3.0 + 3.0 * jax.random.uniform(arg_keys[11], (HEADS,), jnp.float32) ** shard_levels(arg_keys[11], (HEADS,), ((0, 4),), -0.2, 0.2), -3.0, 0.0)
    decay_log = jnp.clip(-1.0 + 2.4 * jax.random.uniform(arg_keys[12], (HEADS,), jnp.float32) ** shard_levels(arg_keys[12], (HEADS,), ((0, 4),), -0.2, 0.2), -1.0, 1.4)
    skip_gain = jnp.clip(jnp.exp(math.log(2.0) - 1.3862944 * jax.random.uniform(arg_keys[13], (HEADS,), jnp.float32) ** shard_levels(arg_keys[13], (HEADS,), ((0, 4),), -0.2, 0.2)), 0.5, 2.0)
    value_taps = centred(arg_keys[14], (CONV, INNER), CONV ** -0.5, 3.0, ((1, 4),))
    write_taps = centred(arg_keys[15], (CONV, GROUPS * STATE), CONV ** -0.5, 3.0, ((1, 4),))
    read_taps = centred(arg_keys[16], (CONV, GROUPS * STATE), CONV ** -0.5, 3.0, ((1, 4),))
    value_window = centred(arg_keys[17], (BATCH, CONV - 1, INNER), 1.0, 6.0, ((0, 8), (2, 4)))
    write_window = centred(arg_keys[18], (BATCH, CONV - 1, GROUPS * STATE), 1.0, 6.0, ((0, 8), (2, 4)))
    read_window = centred(arg_keys[19], (BATCH, CONV - 1, GROUPS * STATE), 1.0, 6.0, ((0, 8), (2, 4)))
    scan_state = centred(arg_keys[20], (BATCH, HEADS, HEAD_DIM, STATE), 0.3, 2.0, ((0, 8), (1, 4)), jnp.float32)
    group_gain = jnp.clip(1.0 + 0.18 * jax.random.normal(arg_keys[21], (INNER,), jnp.float32), 0.099609375, 1.8984375).astype(jnp.bfloat16)
    mixer_out = centred(arg_keys[22], (INNER, D), INNER ** -0.5, 0.0625, ((0, 4), (1, 8)))
    after_gain = jnp.clip(1.0 + 0.18 * jax.random.normal(arg_keys[23], (D,), jnp.float32), 0.099609375, 1.8984375).astype(jnp.bfloat16)
    after_gate = centred(arg_keys[24], (D, FF), D ** -0.5, 0.09375, ((0, 8), (1, 4)))
    after_up = centred(arg_keys[25], (D, FF), D ** -0.5, 0.09375, ((0, 8), (1, 4)))
    after_down = centred(arg_keys[26], (FF, D), FF ** -0.5, 0.0546875, ((0, 4), (1, 8)))
    return dict(block_in=block_in, before_gain=before_gain, before_gate=before_gate, before_up=before_up, before_down=before_down, mix_gain=mix_gain, input_gate=input_gate, input_value=input_value, input_write=input_write, input_read=input_read, input_step=input_step, step_bias=step_bias, decay_log=decay_log, skip_gain=skip_gain, value_taps=value_taps, write_taps=write_taps, read_taps=read_taps, value_window=value_window, write_window=write_window, read_window=read_window, scan_state=scan_state, group_gain=group_gain, mixer_out=mixer_out, after_gain=after_gain, after_gate=after_gate, after_up=after_up, after_down=after_down)


EPS = 1e-06

def half_channel(current, gain_vec, gate_weight, up_weight, down_weight):
    widened = current.astype(jnp.float32)
    row_scale = lax.rsqrt(lax.optimization_barrier(jnp.mean(widened * widened, axis=1, keepdims=True)) + EPS)
    lifted = (widened * gain_vec.astype(jnp.float32)).astype(jnp.bfloat16)
    gate_sum = jnp.dot(lifted, gate_weight, preferred_element_type=jnp.float32) * row_scale
    up_sum = jnp.dot(lifted, up_weight, preferred_element_type=jnp.float32) * row_scale
    hidden = (jax.nn.silu(gate_sum) * up_sum).astype(jnp.bfloat16)
    down_sum = jnp.dot(hidden, down_weight, preferred_element_type=jnp.float32)
    return (widened + 0.5 * down_sum).astype(jnp.bfloat16)

def short_conv(window_state, fresh, taps):
    window = jnp.concatenate([window_state, fresh[:, None, :]], axis=1)
    conv_sum = lax.optimization_barrier(jnp.sum(window.astype(jnp.float32) * taps.astype(jnp.float32)[None], axis=1))
    return (jax.nn.silu(conv_sum), window[:, 1:])

def spread_groups(vectors, heads):
    count = vectors.shape[0]
    groups = vectors.shape[1] // STATE
    shaped = vectors.reshape(count, groups, 1, STATE)
    return jnp.broadcast_to(shaped, (count, groups, heads // groups, STATE)).reshape(count, heads, STATE)

def state_update(gate_rows, value_conv, write_conv, read_conv, step_raw, step_bias, decay_log, skip_gain, scan_state):
    count = value_conv.shape[0]
    heads = step_bias.shape[0]
    step_size = jax.nn.softplus(step_raw + step_bias[None, :])
    decay = jnp.exp(-step_size * jnp.exp(decay_log)[None, :])
    value_heads = value_conv.reshape(count, heads, HEAD_DIM)
    write_heads = spread_groups(write_conv, heads)
    read_heads = spread_groups(read_conv, heads)
    state_next = decay[:, :, None, None] * scan_state + (step_size[:, :, None] * value_heads)[:, :, :, None] * write_heads[:, :, None, :]
    readout = lax.optimization_barrier(jnp.sum(state_next * read_heads[:, :, None, :], axis=3)) + skip_gain[None, :, None] * value_heads
    gated = readout.reshape(count, heads * HEAD_DIM) * jax.nn.silu(gate_rows.astype(jnp.float32))
    groups = write_conv.shape[1] // STATE
    grouped = gated.reshape(count, groups, heads * HEAD_DIM // groups)
    grouped = grouped * lax.rsqrt(lax.optimization_barrier(jnp.mean(grouped * grouped, axis=2, keepdims=True)) + EPS)
    return (grouped.reshape(count, heads * HEAD_DIM), state_next)

def reference(block_in, before_gain, before_gate, before_up, before_down, mix_gain, input_gate, input_value, input_write, input_read, input_step, step_bias, decay_log, skip_gain, value_taps, write_taps, read_taps, value_window, write_window, read_window, scan_state, group_gain, mixer_out, after_gain, after_gate, after_up, after_down):
    first_out = half_channel(block_in, before_gain, before_gate, before_up, before_down)
    widened = first_out.astype(jnp.float32)
    mix_scale = lax.rsqrt(lax.optimization_barrier(jnp.mean(widened * widened, axis=1, keepdims=True)) + EPS)
    lifted = (widened * mix_gain.astype(jnp.float32)).astype(jnp.bfloat16)
    gate_rows = (jnp.dot(lifted, input_gate, preferred_element_type=jnp.float32) * mix_scale).astype(jnp.bfloat16)
    value_fresh = (jnp.dot(lifted, input_value, preferred_element_type=jnp.float32) * mix_scale).astype(jnp.bfloat16)
    write_fresh = (jnp.dot(lifted, input_write, preferred_element_type=jnp.float32) * mix_scale).astype(jnp.bfloat16)
    read_fresh = (jnp.dot(lifted, input_read, preferred_element_type=jnp.float32) * mix_scale).astype(jnp.bfloat16)
    step_raw = jnp.dot(lifted, input_step, preferred_element_type=jnp.float32) * mix_scale
    value_conv, value_next = short_conv(value_window, value_fresh, value_taps)
    write_conv, write_next = short_conv(write_window, write_fresh, write_taps)
    read_conv, read_next = short_conv(read_window, read_fresh, read_taps)
    normed, state_next = state_update(gate_rows, value_conv, write_conv, read_conv, step_raw, step_bias, decay_log, skip_gain, scan_state)
    mixer_rows = (normed * group_gain.astype(jnp.float32)[None, :]).astype(jnp.bfloat16)
    middle = (widened + jnp.dot(mixer_rows, mixer_out, preferred_element_type=jnp.float32)).astype(jnp.bfloat16)
    block_out = half_channel(middle, after_gain, after_gate, after_up, after_down)
    return (block_out, state_next, value_next, write_next, read_next)
```

```python
import functools

import jax
import jax.numpy as jnp
from jax import lax
from jax.experimental import pallas as pl
from jax.experimental.pallas import tpu as pltpu
from jax.sharding import PartitionSpec as P

D = 4096
HEAD_DIM = 64
STATE = 128


EPS = 1e-06

MESH = pl.DeviceIdType.MESH


def greet(axis, n, me):
    barrier = pltpu.get_barrier_semaphore()
    for d in range(1, n):
        pl.semaphore_signal(
            barrier, inc=1, device_id={axis: lax.rem(me + d, n)}, device_id_type=MESH
        )
    pl.semaphore_wait(barrier, n - 1)


def start_scatter(axis, n, me, parts, landed, send_sem, recv_sem):
    copies = []
    for d in range(1, n):
        peer = lax.rem(me + d, n)
        for k, (src, dst) in enumerate(zip(parts, landed)):
            copy = pltpu.make_async_remote_copy(
                src_ref=src.at[peer],
                dst_ref=dst.at[d],
                send_sem=send_sem.at[k, d],
                recv_sem=recv_sem.at[k, d],
                device_id={axis: peer},
                device_id_type=MESH,
            )
            copy.start()
            copies.append(copy)
    return copies


def start_gather(axis, n, me, rows, send_sem, recv_sem):
    copies = []
    for d in range(1, n):
        copy = pltpu.make_async_remote_copy(
            src_ref=rows.at[me],
            dst_ref=rows.at[me],
            send_sem=send_sem.at[d],
            recv_sem=recv_sem.at[d],
            device_id={axis: lax.rem(me + d, n)},
            device_id_type=MESH,
        )
        copy.start()
        copies.append(copy)
    return copies


def finish(copies):
    for copy in copies:
        copy.wait_recv()
    for copy in copies:
        copy.wait_send()


def summed(n, me, own, landed):
    total = own[me].astype(jnp.float32)
    for d in range(1, n):
        total = total + landed[d].astype(jnp.float32)
    return total


def greet_pairs(axis, n, me):
    barrier = pltpu.get_barrier_semaphore()
    pair, _, lines = places(n, me)
    for peer in [pair] + lines[1:]:
        pl.semaphore_signal(barrier, inc=1, device_id={axis: peer}, device_id_type=MESH)
    pl.semaphore_wait(barrier, n // 2)


def places(n, me):
    side, spot, m = lax.rem(me, 2), me // 2, n // 2
    steps = [lax.rem(spot + e, m) for e in range(m)]
    return me + 1 - 2 * side, [2 * q + 1 - side for q in steps], [2 * q + side for q in steps]


def remote(src, dst, send_sem, recv_sem, axis, peer):
    return pltpu.make_async_remote_copy(
        src_ref=src,
        dst_ref=dst,
        send_sem=send_sem,
        recv_sem=recv_sem,
        device_id={axis: peer},
        device_id_type=MESH,
    )


def pair_scatter(axis, n, me, parts, staged, partial, landed, sems):
    pair_send, pair_recv, line_send, line_recv = sems
    pair, across, lines = places(n, me)
    m = n // 2
    first, second = {}, {}
    for k, part in enumerate(parts):
        for e in list(range(1, m)) + [0]:
            first[k, e] = remote(
                part.at[across[e]], staged[k].at[e], pair_send.at[k, e], pair_recv.at[k, e],
                axis, pair,
            )
            first[k, e].start()
    for k, part in enumerate(parts):
        for e in range(1, m):
            first[k, e].wait_recv()
            both = part[lines[e]].astype(jnp.float32) + staged[k][e].astype(jnp.float32)
            partial[k][e] = both.astype(part.dtype)
            second[k, e] = remote(
                partial[k].at[e], landed[k].at[e], line_send.at[k, e], line_recv.at[k, e],
                axis, lines[e],
            )
            second[k, e].start()
    totals = []
    for k, part in enumerate(parts):
        first[k, 0].wait_recv()
        total = part[me].astype(jnp.float32) + staged[k][0].astype(jnp.float32)
        for e in range(1, m):
            second[k, e].wait_recv()
            total = total + landed[k][e].astype(jnp.float32)
        totals.append(total)
    return totals, list(first.values()) + list(second.values())


def pair_gather(axis, n, me, rows, sems):
    pair_send, pair_recv, line_send, line_recv = sems
    pair, _, lines = places(n, me)
    m = n // 2
    side = lax.rem(me, 2)
    sends = []
    own = rows.at[me]
    for e in range(1, m):
        copy = remote(own, own, line_send.at[e], line_recv.at[e], axis, lines[e])
        copy.start()
        sends.append(copy)
    copy = remote(own, own, pair_send.at[0], pair_recv.at[0], axis, pair)
    copy.start()
    passed = [copy]
    for e in range(1, m):
        sends[e - 1].wait_recv()
        came = rows.at[2 * lax.rem(me // 2 + m - e, m) + side]
        copy = remote(came, came, pair_send.at[e], pair_recv.at[e], axis, pair)
        copy.start()
        passed.append(copy)
    for copy in passed:
        copy.wait_recv()
    for copy in sends + passed:
        copy.wait_send()


def gather_kernel(axis, n, own, rows, send_sem, recv_sem):
    me = lax.axis_index(axis)
    rows[me] = own[...]
    greet(axis, n, me)
    finish(start_gather(axis, n, me, rows, send_sem, recv_sem))


def pair_gather_kernel(axis, n, own, rows, *sems):
    me = lax.axis_index(axis)
    rows[me] = own[...]
    greet_pairs(axis, n, me)
    pair_gather(axis, n, me, rows, sems)


def scatter_kernel(axis, n, count, *refs):
    parts, outs, staged, partial, landed = (
        refs[k * count : (k + 1) * count] for k in range(5)
    )
    me = lax.axis_index(axis)
    greet_pairs(axis, n, me)
    totals, copies = pair_scatter(
        axis, n, me, parts, staged, partial, landed, refs[5 * count :]
    )
    for out, total in zip(outs, totals):
        out[...] = total
    for copy in copies:
        copy.wait_send()


def hidden_kernel(axis, n, squares, gate, up, rows, *refs):
    me = lax.axis_index(axis)
    greet_pairs(axis, n, me)
    (square_sum, gate_sum, up_sum), copies = pair_scatter(
        axis, n, me, (squares, gate, up), refs[:3], refs[3:6], refs[6:9], refs[9:13]
    )
    row_scale = lax.rsqrt(square_sum[:, :1] / D + EPS)
    gate_sum = gate_sum * row_scale
    up_sum = up_sum * row_scale
    rows[me] = (gate_sum / (1.0 + jnp.exp(-gate_sum)) * up_sum).astype(rows.dtype)
    pair_gather(axis, n, me, rows, refs[13:])
    for copy in copies:
        copy.wait_send()


def add_kernel(
    axis, n, weight, terms, base, gain, rows, lifted, squares,
    terms_in, send_sem, recv_sem, rows_send, rows_recv,
):
    me = lax.axis_index(axis)
    greet(axis, n, me)
    copies = start_scatter(axis, n, me, (terms,), (terms_in,), send_sem, recv_sem)
    for copy in copies:
        copy.wait_recv()
    returned = summed(n, me, terms, terms_in)
    rows[me] = (base[me].astype(jnp.float32) + weight * returned).astype(rows.dtype)
    gathers = start_gather(axis, n, me, rows, rows_send, rows_recv)
    for copy in copies:
        copy.wait_send()
    finish(gathers)
    for k in range(n):
        widened = rows[k].astype(jnp.float32)
        lifted[k] = (widened * gain[...].astype(jnp.float32)).astype(lifted.dtype)
        total = jnp.sum(widened * widened, axis=1, keepdims=True)
        squares[k] = jnp.broadcast_to(total, squares.shape[1:])


def call(kernel, args, outs, scratch, ident, micros):
    vmem = pl.BlockSpec(memory_space=pltpu.VMEM)
    return pl.pallas_call(
        kernel,
        out_shape=outs,
        in_specs=[vmem] * len(args),
        out_specs=jax.tree.map(lambda _: vmem, outs),
        scratch_shapes=scratch,
        compiler_params=pltpu.CompilerParams(
            collective_id=ident, has_side_effects=True, vmem_limit_bytes=8 * 2**20
        ),
        cost_estimate=pl.CostEstimate(
            flops=0, bytes_accessed=micros * 3_000_000, transcendentals=0
        ),
    )(*args)


def sems(count, *shape):
    return [pltpu.SemaphoreType.DMA(shape)] * count


def gathered(own, axis, ident):
    n = lax.axis_size(axis)
    return call(
        functools.partial(gather_kernel, axis, n),
        (own,),
        jax.ShapeDtypeStruct((n,) + own.shape, own.dtype),
        sems(2, n),
        ident,
        4,
    )


def gathered_pairs(own, axis, ident):
    n = lax.axis_size(axis)
    return call(
        functools.partial(pair_gather_kernel, axis, n),
        (own,),
        jax.ShapeDtypeStruct((n,) + own.shape, own.dtype),
        sems(4, n // 2),
        ident,
        8,
    )


def slots(parts, n):
    return [pltpu.VMEM((n // 2,) + part.shape[1:], part.dtype) for part in parts] * 3


def scattered(parts, axis, ident):
    n = lax.axis_size(axis)
    outs = tuple(jax.ShapeDtypeStruct(part.shape[1:], jnp.float32) for part in parts)
    return call(
        functools.partial(scatter_kernel, axis, n, len(parts)),
        parts,
        outs,
        slots(parts, n) + sems(4, len(parts), n // 2),
        ident,
        14,
    )


def hidden_rows(gate, up, squares, axis, ident):
    n = lax.axis_size(axis)
    return call(
        functools.partial(hidden_kernel, axis, n),
        (squares, gate, up),
        jax.ShapeDtypeStruct(gate.shape, gate.dtype),
        slots((squares, gate, up), n) + sems(4, 3, n // 2) + sems(4, n // 2),
        ident,
        24,
    )


def add_rows(terms, base, weight, gain_vec, axis, ident):
    n = lax.axis_size(axis)
    shape = (n, base.shape[0] // n, base.shape[1])
    rows, lifted, squares = call(
        functools.partial(add_kernel, axis, n, weight),
        (terms.reshape(shape), base.reshape(shape), gain_vec.reshape(1, -1)),
        (
            jax.ShapeDtypeStruct(shape, base.dtype),
            jax.ShapeDtypeStruct(shape, base.dtype),
            jax.ShapeDtypeStruct(shape[:2] + (128,), jnp.float32),
        ),
        [pltpu.VMEM(shape, terms.dtype)] + sems(2, 1, n) + sems(2, n),
        ident,
        7,
    )
    return (
        rows.reshape(base.shape),
        lifted.reshape(base.shape),
        squares.reshape(base.shape[0], 128),
    )


def lifted_rows(rows, gain_vec):
    widened = rows.astype(jnp.float32)
    squares = jnp.sum(widened * widened, axis=1)
    lifted = (widened * gain_vec.astype(jnp.float32)[None, :]).astype(jnp.bfloat16)
    return (lifted, jnp.broadcast_to(squares[:, None], (squares.shape[0], 128)))


def by_rows(array, n):
    return array.reshape(n, array.shape[0] // n, array.shape[1])


def product(rows, weight):
    return jnp.dot(rows, weight, preferred_element_type=jnp.float32)


def half_channel(rows, lifted, squares, gate_weight, up_weight, down_weight, next_gain, ident):
    n = lax.axis_size("kv")
    gate_part = by_rows(product(lifted, gate_weight).astype(jnp.bfloat16), n)
    up_part = by_rows(product(lifted, up_weight).astype(jnp.bfloat16), n)
    hidden = hidden_rows(gate_part, up_part, by_rows(squares, n), "kv", ident)
    hidden = hidden.reshape(rows.shape[0], hidden.shape[2])
    return add_rows(product(hidden, down_weight), rows, 0.5, next_gain, "tp", ident + 1)


def short_conv(window_state, fresh, taps):
    window = jnp.concatenate([window_state, fresh[:, None, :]], axis=1)
    conv_sum = jnp.sum(window.astype(jnp.float32) * taps.astype(jnp.float32)[None], axis=1)
    return (jax.nn.silu(conv_sum), window[:, 1:])


def spread_groups(vectors, heads):
    count = vectors.shape[0]
    groups = vectors.shape[1] // STATE
    shaped = vectors.reshape(count, groups, 1, STATE)
    return jnp.broadcast_to(shaped, (count, groups, heads // groups, STATE)).reshape(
        count, heads, STATE
    )


def state_update(
    gate_rows,
    value_conv,
    write_conv,
    read_conv,
    step_raw,
    step_bias,
    decay_log,
    skip_gain,
    scan_state,
):
    count = value_conv.shape[0]
    heads = step_bias.shape[0]
    step_size = jax.nn.softplus(step_raw + step_bias[None, :])
    decay = jnp.exp(-step_size * jnp.exp(decay_log)[None, :])
    value_heads = value_conv.reshape(count, heads, HEAD_DIM)
    write_heads = spread_groups(write_conv, heads)
    read_heads = spread_groups(read_conv, heads)
    state_next = (
        decay[:, :, None, None] * scan_state
        + (step_size[:, :, None] * value_heads)[:, :, :, None] * write_heads[:, :, None, :]
    )
    readout = (
        jnp.sum(state_next * read_heads[:, :, None, :], axis=3)
        + skip_gain[None, :, None] * value_heads
    )
    gated = readout.reshape(count, heads * HEAD_DIM) * jax.nn.silu(gate_rows.astype(jnp.float32))
    groups = write_conv.shape[1] // STATE
    grouped = gated.reshape(count, groups, heads * HEAD_DIM // groups)
    grouped = grouped * lax.rsqrt(jnp.mean(grouped * grouped, axis=2, keepdims=True) + EPS)
    return (grouped.reshape(count, heads * HEAD_DIM), state_next)


def local(
    block_in,
    before_gain,
    before_gate,
    before_up,
    before_down,
    mix_gain,
    input_gate,
    input_value,
    input_write,
    input_read,
    input_step,
    step_bias,
    decay_log,
    skip_gain,
    value_taps,
    write_taps,
    read_taps,
    value_window,
    write_window,
    read_window,
    scan_state,
    group_gain,
    mixer_out,
    after_gain,
    after_gate,
    after_up,
    after_down,
):
    n = lax.axis_size("kv")
    blocks = gathered(block_in, "tp", 0)
    start = blocks.transpose(1, 0, 2).reshape(blocks.shape[1], -1)
    first_out, lifted, squares = half_channel(
        start, *lifted_rows(start, before_gain), before_gate, before_up, before_down, mix_gain, 1
    )
    parts = [
        by_rows(product(lifted, weight).astype(jnp.bfloat16), n)
        for weight in (input_gate, input_value, input_write, input_read)
    ]
    heads = input_step.shape[1]
    step_weight = jnp.pad(input_step, ((0, 0), (0, -heads % 128)))
    square_sum, gate_sum, value_sum, write_sum, read_sum, step_sum = scattered(
        (by_rows(squares, n),) + tuple(parts) + (by_rows(product(lifted, step_weight), n),),
        "kv",
        3,
    )
    step_sum, totals = step_sum[:, :heads], square_sum[:, 0]
    mix_scale = lax.rsqrt(totals / D + EPS)[:, None]
    gate_rows = (gate_sum * mix_scale).astype(jnp.bfloat16)
    value_fresh = (value_sum * mix_scale).astype(jnp.bfloat16)
    write_fresh = (write_sum * mix_scale).astype(jnp.bfloat16)
    read_fresh = (read_sum * mix_scale).astype(jnp.bfloat16)
    step_raw = step_sum * mix_scale
    value_conv, value_next = short_conv(value_window, value_fresh, value_taps)
    write_conv, write_next = short_conv(write_window, write_fresh, write_taps)
    read_conv, read_next = short_conv(read_window, read_fresh, read_taps)
    normed, state_next = state_update(
        gate_rows,
        value_conv,
        write_conv,
        read_conv,
        step_raw,
        step_bias,
        decay_log,
        skip_gain,
        scan_state,
    )
    mixer_rows = (normed * group_gain.astype(jnp.float32)[None, :]).astype(jnp.bfloat16)
    mixer_all = gathered_pairs(mixer_rows, "kv", 4)
    back_part = product(mixer_all.reshape(-1, mixer_all.shape[2]), mixer_out)
    middle, lifted, squares = add_rows(back_part, first_out, 1.0, after_gain, "tp", 5)
    last, _, _ = half_channel(
        middle, lifted, squares, after_gate, after_up, after_down, after_gain, 6
    )
    width = block_in.shape[1]
    block_out = lax.dynamic_slice_in_dim(last, lax.axis_index("tp") * width, width, 1)
    return (block_out, state_next, value_next, write_next, read_next)


def solution(mesh):
    placed = (
        P(None, ("kv", "tp")),
        P("kv"),
        P("kv", "tp"),
        P("kv", "tp"),
        P("tp", "kv"),
        P("kv"),
        P("kv", "tp"),
        P("kv", "tp"),
        P("kv", "tp"),
        P("kv", "tp"),
        P("kv", "tp"),
        P("tp"),
        P("tp"),
        P("tp"),
        P(None, "tp"),
        P(None, "tp"),
        P(None, "tp"),
        P("kv", None, "tp"),
        P("kv", None, "tp"),
        P("kv", None, "tp"),
        P("kv", "tp", None, None),
        P("tp"),
        P("tp", "kv"),
        P("kv"),
        P("kv", "tp"),
        P("kv", "tp"),
        P("tp", "kv"),
    )
    return jax.shard_map(
        local,
        mesh=mesh,
        in_specs=placed,
        out_specs=(
            P(None, ("kv", "tp")),
            P("kv", "tp", None, None),
            P("kv", None, "tp"),
            P("kv", None, "tp"),
            P("kv", None, "tp"),
        ),
        check_vma=False,
    )
```
